32 devices in a mesh: sp: 16 (over z, y, core), tp: 2 (over x).
Axes of the slice: x: 2, y: 2, z: 4, core: 2. Of those that a mesh axis runs over, the one named last changes fastest.
Arguments:
- query_rows: bfloat16 [10240, 1536], P('sp', 'tp'), may hold values from -8 to 8
- key_rows: bfloat16 [10240, 1536], P('sp', 'tp'), may hold values from -8 to 8
- value_rows: bfloat16 [10240, 1536], P('sp', 'tp'), may hold values from -6 to 6
- query_gain: bfloat16 [64], replicated, may hold values from 0.25 to 4.2
- key_gain: bfloat16 [64], replicated, may hold values from 0.25 to 4.2
- position_bias: bfloat16 [24, 320], P('tp'), may hold values from -165 to 3
- output_grad: bfloat16 [10240, 1536], P('sp', 'tp'), may hold values from -24 to 24
Outputs:
- query_grad: bfloat16 [10240, 1536], P('sp', 'tp')
- key_grad: bfloat16 [10240, 1536], P('sp', 'tp')
- value_grad: bfloat16 [10240, 1536], P('sp', 'tp')
- bias_grad: float32 [24, 320], P('tp')
- query_gain_grad: float32 [64], replicated
- key_gain_grad: float32 [64], replicated
The draws below stay inside these ranges and needn't reach their ends.
All inputs are finite; a program needn't handle non-finite values.
Results may differ from the reference program's by a relative error of at most 0.0055.
The reference program's roundings to bfloat16 on the way count: a program that leaves them out, or rounds other values in their place, can miss the bound.
Values may be sent and summed in bfloat16 or wider, within the bound.
A program may use at most 128 MiB of HBM per device.

```python
import jax
import jax.numpy as jnp
import numpy as np
from jax import lax

HEADS = 24
HEAD_DIM = 64
SEG = 64
LEFT = 8
CLIP = 256
TOK_DEV = 640
SEQ = 10240


def planted_pair(base):
    key_part = jax.random.normal(jax.random.fold_in(base, 101), (SEQ, HEADS * HEAD_DIM), jnp.float32)
    query_part = jax.random.normal(jax.random.fold_in(base, 202), (SEQ, HEADS * HEAD_DIM), jnp.float32)
    return (jnp.clip(query_part, -8.0, 8.0), jnp.clip(key_part, -8.0, 8.0))


def draw_query_rows(key, part):
    return planted_pair(key)[0].astype(jnp.bfloat16)


def draw_key_rows(key, part):
    return planted_pair(key)[1].astype(jnp.bfloat16)


def gain_of(base, salt):
    return 1.0 + 0.18 * jnp.clip(jax.random.normal(jax.random.fold_in(base, salt), (HEAD_DIM,), jnp.float32), -4.0, 4.0)


def draw_query_gain(key, part):
    return gain_of(key, 505).astype(jnp.bfloat16)


def draw_key_gain(key, part):
    return gain_of(key, 606).astype(jnp.bfloat16)


def draw_position_bias(key, part):
    table = 0.5 * jnp.clip(jax.random.normal(jax.random.fold_in(key, 808), (HEADS, CLIP + SEG), jnp.float32), -6.0, 6.0)
    return table.astype(jnp.bfloat16)


def shard_levels(rng, extent, shards, least, largest):
    def one(dim, shards_of):
        steps = jax.random.uniform(jax.random.fold_in(jax.random.fold_in(rng, 6), dim), (shards_of,), jnp.float32, least / len(shards), largest / len(shards))
        return jnp.repeat(jnp.exp(steps), extent[dim] // shards_of).reshape((-1,) + (1,) * (len(extent) - dim - 1))

    gain = one(*shards[0])
    for cut in shards[1:]:
        gain = gain * one(*cut)
    return gain


def gaussian(rng, extent, spread, bound, shards=(), held_as=jnp.bfloat16):
    drawn = spread * jax.random.normal(rng, extent, jnp.float32)
    if shards:
        drawn = drawn * shard_levels(rng, extent, shards, -0.22, 0.18)
    return jnp.clip(drawn, -bound, bound).astype(held_as)


def setup_inputs(seed: int = 0) -> dict:
    key_of = jax.random.split(jax.random.key(seed), 8)
    query_rows = draw_query_rows(jax.random.fold_in(key_of[7], 71), 0)
    key_rows = draw_key_rows(jax.random.fold_in(key_of[7], 71), 0)
    value_rows = gaussian(key_of[2], (SEQ, HEADS * HEAD_DIM), 1.0, 6.0, ((0, 16), (1, 2)))
    query_gain = draw_query_gain(jax.random.fold_in(key_of[7], 71), 0)
    key_gain = draw_key_gain(jax.random.fold_in(key_of[7], 71), 0)
    position_bias = draw_position_bias(jax.random.fold_in(key_of[7], 71), 0)
    output_grad = gaussian(key_of[6], (SEQ, HEADS * HEAD_DIM), 4.0, 24.0, ((0, 16), (1, 2)))
    return {"query_rows": query_rows, "key_rows": key_rows, "value_rows": value_rows, "query_gain": query_gain, "key_gain": key_gain, "position_bias": position_bias, "output_grad": output_grad}


NORM_EPS = 1e-06

def unit_rows(values):
    widened = values.astype(jnp.float32)
    scale_rows = lax.rsqrt(lax.optimization_barrier(jnp.mean(widened * widened, axis=-1, keepdims=True)) + NORM_EPS)
    return (widened * scale_rows, scale_rows)

def band_of(segments, seg_count):
    return jnp.concatenate([segments[offset:offset + seg_count] for offset in range(LEFT + 1)], axis=1)

def unband(banded, seg_count):
    summed = jnp.zeros((seg_count + LEFT, SEG) + banded.shape[2:], jnp.float32)
    for offset in range(LEFT + 1):
        summed = summed.at[offset:offset + seg_count].add(banded[:, offset * SEG:(offset + 1) * SEG])
    return summed

def layout(seg_count):
    band_pos = np.repeat(np.arange(LEFT + 1), SEG)
    key_pos = np.tile(np.arange(SEG), LEFT + 1)
    query_pos = np.arange(SEG)[:, None]
    distance = (LEFT - band_pos)[None, :] * SEG + query_pos - key_pos[None, :]
    bias_index = (np.minimum(distance, CLIP) + SEG - 1).astype(np.int32)
    visible = np.arange(seg_count)[:, None] - LEFT + band_pos[None, :] >= 0
    segs_block = TOK_DEV // SEG
    query_seg_index = np.arange(seg_count)[:, None]
    key_seg_index = query_seg_index - LEFT + band_pos[None, :]
    crossing = (query_seg_index // segs_block != key_seg_index // segs_block).astype(np.float32)
    return (bias_index, visible, crossing)

def split_unband(banded, crossing, seg_count):
    cross_mask = jnp.asarray(crossing)[:, :, None]
    own_part = unband(banded * (1.0 - cross_mask), seg_count)[LEFT:].reshape(SEQ, HEAD_DIM)
    cross_part = unband(banded * cross_mask, seg_count)[LEFT:].reshape(SEQ, HEAD_DIM)
    cross_low = lax.optimization_barrier(cross_part.astype(jnp.bfloat16)).astype(jnp.float32)
    return own_part + cross_low

def reference(query_rows, key_rows, value_rows, query_gain, key_gain, position_bias, output_grad):
    seg_count = SEQ // SEG
    bias_index, visible, crossing = layout(seg_count)
    score_scale = HEAD_DIM ** (-0.5)
    gain_query = query_gain.astype(jnp.float32)
    gain_key = key_gain.astype(jnp.float32)

    def by_head(matrix):
        return matrix.reshape(SEQ, HEADS, HEAD_DIM).transpose(1, 0, 2)

    def one_head(inputs):
        query_head, key_head, value_head, grad_head, bias_table = inputs
        query_hat, query_scale = unit_rows(query_head)
        key_hat, key_scale = unit_rows(key_head)
        query_unit = lax.optimization_barrier((query_hat * gain_query).astype(jnp.bfloat16))
        key_unit = lax.optimization_barrier((key_hat * gain_key).astype(jnp.bfloat16))
        padding = jnp.zeros((LEFT * SEG, HEAD_DIM), jnp.bfloat16)
        key_band = band_of(jnp.concatenate([padding, key_unit], 0).reshape(seg_count + LEFT, SEG, HEAD_DIM), seg_count).astype(jnp.float32)
        value_band = band_of(jnp.concatenate([padding, value_head], 0).reshape(seg_count + LEFT, SEG, HEAD_DIM), seg_count).astype(jnp.float32)
        query_seg = query_unit.reshape(seg_count, SEG, HEAD_DIM).astype(jnp.float32)
        grad_seg = grad_head.reshape(seg_count, SEG, HEAD_DIM).astype(jnp.float32)
        row_bias = bias_table.astype(jnp.float32)[bias_index]
        scores = jnp.einsum('cqd,ckd->cqk', query_seg, key_band) * score_scale + row_bias[None]
        scores = jnp.where(visible[:, None, :], scores, -jnp.inf)
        row_peak = lax.optimization_barrier(jnp.max(scores, axis=-1, keepdims=True))
        raised = jnp.exp(scores - row_peak)
        weights = raised / lax.optimization_barrier(jnp.sum(raised, axis=-1, keepdims=True))
        weights_low = lax.optimization_barrier(weights.astype(jnp.bfloat16)).astype(jnp.float32)
        d_weights = jnp.einsum('cqd,ckd->cqk', grad_seg, value_band)
        row_delta = lax.optimization_barrier(jnp.sum(weights * d_weights, axis=-1, keepdims=True))
        d_scores = weights * (d_weights - row_delta)
        d_low = lax.optimization_barrier(d_scores.astype(jnp.bfloat16)).astype(jnp.float32)
        dq_unit = (jnp.einsum('cqk,ckd->cqd', d_low, key_band) * score_scale).reshape(SEQ, HEAD_DIM)
        dk_unit = split_unband(jnp.einsum('cqk,cqd->ckd', d_low, query_seg) * score_scale, crossing, seg_count)
        value_grad = split_unband(jnp.einsum('cqk,cqd->ckd', weights_low, grad_seg), crossing, seg_count)
        bias_grad = jnp.zeros((CLIP + SEG,), jnp.float32).at[bias_index.ravel()].add(lax.optimization_barrier(jnp.sum(d_scores, axis=0)).ravel())
        dq_scaled = dq_unit * gain_query
        query_grad = query_scale * (dq_scaled - query_hat * lax.optimization_barrier(jnp.mean(dq_scaled * query_hat, axis=-1, keepdims=True)))
        dk_scaled = dk_unit * gain_key
        key_grad = key_scale * (dk_scaled - key_hat * lax.optimization_barrier(jnp.mean(dk_scaled * key_hat, axis=-1, keepdims=True)))
        return (query_grad.astype(jnp.bfloat16), key_grad.astype(jnp.bfloat16), value_grad.astype(jnp.bfloat16), bias_grad, lax.optimization_barrier(jnp.sum(dq_unit * query_hat, axis=0)), lax.optimization_barrier(jnp.sum(dk_unit * key_hat, axis=0)))
    results = lax.map(one_head, (by_head(query_rows), by_head(key_rows), by_head(value_rows), by_head(output_grad), position_bias))

    def to_rows(stacked):
        return stacked.transpose(1, 0, 2).reshape(SEQ, HEADS * HEAD_DIM)
    return (to_rows(results[0]), to_rows(results[1]), to_rows(results[2]), results[3], lax.optimization_barrier(jnp.sum(results[4], axis=0)), lax.optimization_barrier(jnp.sum(results[5], axis=0)))
```

```python
import functools

import jax
import jax.numpy as jnp
from jax import lax
from jax.experimental import pallas as pl
from jax.experimental.pallas import tpu as pltpu
from jax.sharding import PartitionSpec as P

SEG = 64
LEFT = 8
REACH = SEG * LEFT
RSPAN = 320
NORM_EPS = 1e-06
BLK = 2 * SEG
BAND = REACH + BLK
NEG = -1e30
F32 = jnp.float32
BF16 = jnp.bfloat16


def dot(a, b, dims):
    return lax.dot_general(a, b, (dims, ((), ())), preferred_element_type=F32)


def half_ones():
    row = lax.broadcasted_iota(jnp.int32, (BLK, BLK), 0) // 64
    col = lax.broadcasted_iota(jnp.int32, (BLK, BLK), 1) // 64
    return jnp.where(row == col, 1.0, 0.0).astype(BF16)


def head_mean(x, ones):
    high = x.astype(BF16)
    low = (x - high.astype(F32)).astype(BF16)
    return (dot(high, ones, ((1,), (0,))) + dot(low, ones, ((1,), (0,)))) * (1.0 / 64.0)


def normed(rows, ones):
    wide = rows.astype(F32)
    scale = lax.rsqrt(head_mean(wide * wide, ones) + NORM_EPS)
    return wide * scale, scale


def norm_grad(d_unit, gain, hat, scale, ones):
    scaled = d_unit * gain
    return scale * (scaled - hat * head_mean(scaled * hat, ones))


def stack_halves(x):
    lane = lax.broadcasted_iota(jnp.int32, x.shape, 1)
    zero = jnp.zeros_like(x)
    return jnp.concatenate([jnp.where(lane < 64, x, zero), jnp.where(lane < 64, zero, x)], axis=0)


def build_bias(table_row, bias_ref, head):
    wide = jnp.broadcast_to(table_row, (8, 512))
    sub = lax.broadcasted_iota(jnp.int32, (8, 512), 0)
    for bit in (1, 2, 4):
        wide = jnp.where((sub & bit) != 0, pltpu.roll(wide, bit, 1), wide)
    half = 8
    while half < BLK:
        wide = jnp.concatenate([wide, pltpu.roll(wide, half, 1)], axis=0)
        half *= 2
    lanes = slice(head * BLK, (head + 1) * BLK)
    row = lax.broadcasted_iota(jnp.int32, (BLK, BLK), 0)
    col = lax.broadcasted_iota(jnp.int32, (BLK, BLK), 1)
    far = jnp.broadcast_to(table_row[:, 0:1], (BLK, BLK))
    bias_ref[0:BLK, lanes] = jnp.where((row < SEG) & (col >= SEG), NEG, far)
    bias_ref[BLK : 2 * BLK, lanes] = far
    for j in range(3):
        tile = wide[:, ((4 - j) % 4) * BLK : ((4 - j) % 4) * BLK + BLK]
        if j == 2:
            tile = jnp.where((row >= SEG) & (col < SEG), NEG, tile)
        bias_ref[(2 + j) * BLK : (3 + j) * BLK, lanes] = tile


def fold_bias(acc_ref, head):
    lanes = slice(head * BLK, (head + 1) * BLK)
    tiles = [acc_ref[j * BLK : (j + 1) * BLK, lanes] for j in range(3)]
    wide = jnp.concatenate([tiles[0], jnp.zeros_like(tiles[0]), tiles[2], tiles[1]], axis=1)
    half = BLK // 2
    while half >= 8:
        wide = wide[:half] + pltpu.roll(wide[half:], 512 - half, 1)
        half //= 2
    for half in (4, 2, 1):
        wide = wide + pltpu.roll(pltpu.roll(wide, 512 - half, 1), 8 - half, 0)
    return wide[0:1]


def attend(refs, first, blocks, ones, gain_q):
    (q_ref, g_ref, qg_ref, gq_ref, clip_ref, k_s, kt_s, v_s, bias_s, acc_s, s_s, dw_s, w_s, ds_s, dk_s, dv_s) = refs

    def block(i, _):
        base = pl.multiple_of(i * BLK, BLK)
        rows = pl.ds(base, BLK)
        hat, scale = normed(q_ref[rows, :], ones)
        qs = stack_halves((hat * gain_q).astype(BF16) * jnp.asarray(0.125, BF16))
        gs = stack_halves(g_ref[rows, :])
        peaks, penalties = [], []
        for j in range(5):
            keys = pl.ds(base + j * BLK, BLK)
            own = slice(j * BLK, (j + 1) * BLK)
            s = dot(k_s[keys, :], qs, ((1,), (1,))) + bias_s[own, :]
            s_s[own, :] = s
            dw_s[own, :] = dot(v_s[keys, :], gs, ((1,), (1,)))
            penalty = jnp.where(first & (j < 4 - i), NEG, 0.0)
            penalties.append(penalty)
            peaks.append(jnp.max(s, axis=0, keepdims=True) + penalty)
        peak = functools.reduce(jnp.maximum, peaks)
        total = jnp.zeros((1, 2 * BLK), F32)
        delta = jnp.zeros((1, 2 * BLK), F32)
        for j in range(5):
            own = slice(j * BLK, (j + 1) * BLK)
            e = jnp.exp(s_s[own, :] - (peak - penalties[j]))
            s_s[own, :] = e
            total = total + jnp.sum(e, axis=0, keepdims=True)
            delta = delta + jnp.sum(e * dw_s[own, :], axis=0, keepdims=True)
        inverse = 1.0 / total
        delta = delta * inverse
        clipped = jnp.zeros((1, 2 * BLK), F32)
        for j in range(5):
            own = slice(j * BLK, (j + 1) * BLK)
            keys = pl.ds(base + j * BLK, BLK)
            w = s_s[own, :] * inverse
            ds = w * (dw_s[own, :] - delta)
            if j < 2:
                clipped = clipped + jnp.sum(ds, axis=0, keepdims=True)
            else:
                acc_s[(j - 2) * BLK : (j - 1) * BLK, :] += ds
            w_low = w.astype(BF16)
            ds_low = ds.astype(BF16)
            ds_s[own, :] = ds_low
            dk_s[keys, :] += dot(ds_low, qs, ((1,), (0,)))
            dv_s[keys, :] += dot(w_low, gs, ((1,), (0,)))
        clip_ref[...] += clipped
        dqt = dot(kt_s[:, pl.ds(base, BAND)], ds_s[...], ((1,), (0,)))
        dqt = jnp.concatenate([dqt[:64, :BLK], dqt[64:, BLK:]], axis=0)
        dq = dqt.T * 0.125
        gq_ref[...] += jnp.sum(dq * hat, axis=0, keepdims=True)
        qg_ref[rows, :] = norm_grad(dq, gain_q, hat, scale, ones).astype(BF16)
        return 0

    lax.fori_loop(0, blocks, block, 0)


def main_kernel(
    q_ref, k_ref, v_ref, g_ref, pk_ref, pv_ref, gains_ref, table_ref,
    qg_ref, dk_ref, dv_ref, ck_ref, cv_ref, bg_ref, clip_ref, gq_ref,
    k_s, kt_s, v_s, bias_s, acc_s, s_s, dw_s, w_s, ds_s, dk_s, dv_s,
):
    tokens = q_ref.shape[0]
    first = lax.axis_index("sp") == 0
    ones = half_ones()
    gain_q = gains_ref[0:1, :]
    gain_k = gains_ref[1:2, :]
    for b in range((tokens + REACH) // BLK):
        raw = pk_ref[b * BLK : (b + 1) * BLK, :] if b < 4 else k_ref[(b - 4) * BLK : (b - 3) * BLK, :]
        unit = normed(raw, ones)[0] * gain_k
        k_s[b * BLK : (b + 1) * BLK, :] = unit.astype(BF16)
        kt_s[:, b * BLK : (b + 1) * BLK] = unit.T.astype(BF16)
    v_s[:REACH, :] = pv_ref[...]
    v_s[REACH:, :] = v_ref[...]
    dk_s[...] = jnp.zeros_like(dk_s)
    dv_s[...] = jnp.zeros_like(dv_s)
    acc_s[...] = jnp.zeros_like(acc_s)
    clip_ref[...] = jnp.zeros_like(clip_ref)
    gq_ref[...] = jnp.zeros_like(gq_ref)
    for head in range(2):
        build_bias(table_ref[head : head + 1, :], bias_s, head)
    attend(
        (q_ref, g_ref, qg_ref, gq_ref, clip_ref, k_s, kt_s, v_s, bias_s, acc_s, s_s, dw_s, w_s, ds_s, dk_s, dv_s),
        first, tokens // BLK, ones, gain_q,
    )
    for head in range(2):
        bg_ref[head : head + 1, :] = fold_bias(acc_s, head)
    ck_ref[...] = dk_s[:REACH, :].astype(BF16)
    cv_ref[...] = dv_s[:REACH, :].astype(BF16)
    dk_ref[...] = dk_s[REACH:, :]
    dv_ref[...] = dv_s[REACH:, :]


def final_kernel(k_ref, dk_ref, dv_ref, bk_ref, bv_ref, gains_ref, kg_ref, vg_ref, gk_ref):
    tokens = k_ref.shape[0]
    ones = half_ones()
    gain_k = gains_ref[1:2, :]
    total = jnp.zeros((1, BLK), F32)
    for b in range(tokens // BLK):
        rows = slice(b * BLK, (b + 1) * BLK)
        hat, scale = normed(k_ref[rows, :], ones)
        dk, dv = dk_ref[rows, :], dv_ref[rows, :]
        back = b * BLK - (tokens - REACH)
        if back >= 0:
            dk = dk + bk_ref[back : back + BLK, :].astype(F32)
            dv = dv + bv_ref[back : back + BLK, :].astype(F32)
        total = total + jnp.sum(dk * hat, axis=0, keepdims=True)
        kg_ref[rows, :] = norm_grad(dk, gain_k, hat, scale, ones).astype(BF16)
        vg_ref[rows, :] = dv.astype(BF16)
    gk_ref[...] = total


def passed_along(block, axis, distance):
    devices = range(lax.axis_size(axis))
    route = [(i - distance, i) for i in devices if i - distance in devices]
    return lax.ppermute(block, axis, route)


def body(query_rows, key_rows, value_rows, query_gain, key_gain, position_bias, output_grad):
    heads = position_bias.shape[0]
    pairs = heads // 2
    tokens = query_rows.shape[0]
    table = position_bias.astype(F32)
    last = jnp.broadcast_to(table[:, -1:], (heads, 129))
    table = jnp.concatenate([last, jnp.full((heads, 64), NEG, F32), table[:, :-1]], axis=1)
    table = table.reshape(pairs, 2, 512)
    gains = jnp.stack([jnp.tile(query_gain.astype(F32), 2), jnp.tile(key_gain.astype(F32), 2)])
    prior_key, prior_value = passed_along((key_rows[tokens - REACH :], value_rows[tokens - REACH :]), "sp", 1)

    full = pl.BlockSpec((tokens, BLK), lambda p: (0, p))
    reach = pl.BlockSpec((REACH, BLK), lambda p: (0, p))
    small = pl.BlockSpec((2, BLK), lambda p: (0, 0))

    def per_pair(rows, lanes):
        return pl.BlockSpec((None, rows, lanes), lambda p: (p, 0, 0))

    def shape(rows, dtype):
        return jax.ShapeDtypeStruct((rows, heads * 64), dtype)

    flops = pairs * tokens * 2 * 5 * 2 * BAND * 128
    ext = tokens + REACH
    query_grad, dk_own, dv_own, cross_k, cross_v, fold, clip, gq = pl.pallas_call(
        main_kernel,
        grid=(pairs,),
        in_specs=[full, full, full, full, reach, reach, small, per_pair(2, 512)],
        out_specs=[full, full, full, reach, reach, per_pair(2, 512), per_pair(1, 2 * BLK), per_pair(1, BLK)],
        out_shape=[
            shape(tokens, BF16), shape(tokens, F32), shape(tokens, F32), shape(REACH, BF16), shape(REACH, BF16),
            jax.ShapeDtypeStruct((pairs, 2, 512), F32),
            jax.ShapeDtypeStruct((pairs, 1, 2 * BLK), F32),
            jax.ShapeDtypeStruct((pairs, 1, BLK), F32),
        ],
        scratch_shapes=[
            pltpu.VMEM((ext, BLK), BF16), pltpu.VMEM((BLK, ext), BF16), pltpu.VMEM((ext, BLK), BF16),
            pltpu.VMEM((BAND, 2 * BLK), F32), pltpu.VMEM((3 * BLK, 2 * BLK), F32),
            pltpu.VMEM((BAND, 2 * BLK), F32), pltpu.VMEM((BAND, 2 * BLK), F32),
            pltpu.VMEM((BAND, 2 * BLK), BF16), pltpu.VMEM((BAND, 2 * BLK), BF16),
            pltpu.VMEM((ext, BLK), F32), pltpu.VMEM((ext, BLK), F32),
        ],
        cost_estimate=pl.CostEstimate(flops=flops, bytes_accessed=14_000_000, transcendentals=pairs * tokens * BAND),
        name="attend",
    )(query_rows, key_rows, value_rows, output_grad, prior_key, prior_value, gains, table)

    back_k, back_v = passed_along((cross_k, cross_v), "sp", -1)
    key_grad, value_grad, gk = pl.pallas_call(
        final_kernel,
        grid=(pairs,),
        in_specs=[full, full, full, reach, reach, small],
        out_specs=[full, full, per_pair(1, BLK)],
        out_shape=[shape(tokens, BF16), shape(tokens, BF16), jax.ShapeDtypeStruct((pairs, 1, BLK), F32)],
        name="finish",
    )(key_rows, dk_own, dv_own, back_k, back_v, gains)

    fold = fold.reshape(heads, 512)
    clip = jnp.sum(clip.reshape(heads, BLK), axis=1, keepdims=True)
    bias_part = jnp.concatenate([fold[:, 193:], jnp.sum(fold[:, :129], axis=1, keepdims=True) + clip], axis=1)
    gain_part = jnp.stack([jnp.sum(x.reshape(-1, 64), axis=0) for x in (gq, gk)])
    bias_grad = lax.psum(bias_part, "sp")
    gain_grad = lax.psum(gain_part, ("sp", "tp"))
    return (query_grad, key_grad, value_grad, bias_grad, gain_grad[0], gain_grad[1])


def solution(mesh):
    placed = (P("sp", "tp"), P("sp", "tp"), P("sp", "tp"), P(), P(), P("tp", None), P("sp", "tp"))
    return jax.shard_map(
        body,
        mesh=mesh,
        in_specs=placed,
        out_specs=(P("sp", "tp"), P("sp", "tp"), P("sp", "tp"), P("tp", None), P(), P()),
        check_vma=False,
    )
```

```python
import functools

import jax
import jax.numpy as jnp
from jax import lax
from jax.experimental import pallas as pl
from jax.experimental.pallas import tpu as pltpu
from jax.sharding import PartitionSpec as P

SEG = 64
LEFT = 8
REACH = SEG * LEFT
RSPAN = 320
NORM_EPS = 1e-06
BLK = 2 * SEG
BAND = REACH + BLK
NEG = -1e30
F32 = jnp.float32
BF16 = jnp.bfloat16


def dot(a, b, dims):
    return lax.dot_general(a, b, (dims, ((), ())), preferred_element_type=F32)


def half_ones():
    row = lax.broadcasted_iota(jnp.int32, (BLK, BLK), 0) // 64
    col = lax.broadcasted_iota(jnp.int32, (BLK, BLK), 1) // 64
    return jnp.where(row == col, 1.0, 0.0).astype(BF16)


def head_mean(x, ones):
    high = x.astype(BF16)
    low = (x - high.astype(F32)).astype(BF16)
    return (dot(high, ones, ((1,), (0,))) + dot(low, ones, ((1,), (0,)))) * (1.0 / 64.0)


def normed(rows, ones):
    wide = rows.astype(F32)
    scale = lax.rsqrt(head_mean(wide * wide, ones) + NORM_EPS)
    return wide * scale, scale


def norm_grad(d_unit, gain, hat, scale, ones):
    scaled = d_unit * gain
    return scale * (scaled - hat * head_mean(scaled * hat, ones))


def stack_halves(x):
    lane = lax.broadcasted_iota(jnp.int32, x.shape, 1)
    zero = jnp.zeros_like(x)
    return jnp.concatenate([jnp.where(lane < 64, x, zero), jnp.where(lane < 64, zero, x)], axis=0)


def build_bias(table_row, bias_ref, head):
    wide = jnp.broadcast_to(table_row, (8, 512))
    sub = lax.broadcasted_iota(jnp.int32, (8, 512), 0)
    for bit in (1, 2, 4):
        wide = jnp.where((sub & bit) != 0, pltpu.roll(wide, bit, 1), wide)
    half = 8
    while half < BLK:
        wide = jnp.concatenate([wide, pltpu.roll(wide, half, 1)], axis=0)
        half *= 2
    lanes = slice(head * BLK, (head + 1) * BLK)
    row = lax.broadcasted_iota(jnp.int32, (BLK, BLK), 0)
    col = lax.broadcasted_iota(jnp.int32, (BLK, BLK), 1)
    far = jnp.broadcast_to(table_row[:, 0:1], (BLK, BLK))
    bias_ref[0:BLK, lanes] = jnp.where((row < SEG) & (col >= SEG), NEG, far)
    bias_ref[BLK : 2 * BLK, lanes] = far
    for j in range(3):
        tile = wide[:, ((4 - j) % 4) * BLK : ((4 - j) % 4) * BLK + BLK]
        if j == 2:
            tile = jnp.where((row >= SEG) & (col < SEG), NEG, tile)
        bias_ref[(2 + j) * BLK : (3 + j) * BLK, lanes] = tile


def fold_bias(acc_ref, head):
    lanes = slice(head * BLK, (head + 1) * BLK)
    tiles = [acc_ref[j * BLK : (j + 1) * BLK, lanes] for j in range(3)]
    wide = jnp.concatenate([tiles[0], jnp.zeros_like(tiles[0]), tiles[2], tiles[1]], axis=1)
    half = BLK // 2
    while half >= 8:
        wide = wide[:half] + pltpu.roll(wide[half:], 512 - half, 1)
        half //= 2
    for half in (4, 2, 1):
        wide = wide + pltpu.roll(pltpu.roll(wide, 512 - half, 1), 8 - half, 0)
    return wide[0:1]


def flip(index, distance):
    return index + distance * (1 - 2 * ((index // distance) % 2))


def doubling(size):
    return [1 << r for r in range(size.bit_length() - 1)]


def kernel(
    sp, tp, q_ref, k_ref, v_ref, g_ref, gains_ref, table_ref,
    qg_ref, kg_ref, vg_ref, out_ref,
    k_s, kt_s, v_s, bias_s, acc_s, s_s, dw_s, ds_s, dk_s, dv_s, clip_s, gq_s, gk_s,
    pk_s, pv_s, ck_s, cv_s, bk_s, bv_s, stat_s, got_s,
    prior_send, prior_recv, cross_send, cross_recv, stat_send, stat_recv,
):
    tokens = q_ref.shape[0]
    blocks = tokens // BLK
    pairs = pk_s.shape[0]
    me = lax.axis_index("sp")
    me_tp = lax.axis_index("tp")
    right, left = lax.rem(me + 1, sp), lax.rem(me + sp - 1, sp)
    partners = [{"sp": flip(me, d)} for d in doubling(sp)] + [{"tp": flip(me_tp, d)} for d in doubling(tp)]
    first = me == 0

    barrier = pltpu.get_barrier_semaphore()
    greeted = [{"sp": right}, {"sp": left}] + partners
    for device in greeted:
        pl.semaphore_signal(barrier, inc=1, device_id=device, device_id_type=pl.DeviceIdType.MESH)
    pl.semaphore_wait(barrier, len(greeted))

    def remote(src, dst, send, recv, device):
        return pltpu.make_async_remote_copy(
            src_ref=src, dst_ref=dst, send_sem=send, recv_sem=recv,
            device_id=device, device_id_type=pl.DeviceIdType.MESH,
        )

    def lanes_of(p):
        return pl.ds(pl.multiple_of(p * BLK, BLK), BLK)

    def prior_copies(p):
        rows = slice(tokens - REACH, tokens)
        return (
            remote(k_ref.at[rows, lanes_of(p)], pk_s.at[p], prior_send.at[0, p], prior_recv.at[0, p], {"sp": right}),
            remote(v_ref.at[rows, lanes_of(p)], pv_s.at[p], prior_send.at[1, p], prior_recv.at[1, p], {"sp": right}),
        )

    def cross_copies(p):
        return (
            remote(ck_s.at[p], bk_s.at[p], cross_send.at[0, p], cross_recv.at[0, p], {"sp": left}),
            remote(cv_s.at[p], bv_s.at[p], cross_send.at[1, p], cross_recv.at[1, p], {"sp": left}),
        )

    for p in range(pairs):
        for copy in prior_copies(p):
            copy.start()

    ones = half_ones()
    gain_q = gains_ref[0:1, :]
    gain_k = gains_ref[1:2, :]
    stat_s[0] = jnp.zeros(stat_s.shape[1:], F32)
    gq_s[...] = jnp.zeros_like(gq_s)
    gk_s[...] = jnp.zeros_like(gk_s)

    def key_tile(raw, b):
        unit = normed(raw, ones)[0] * gain_k
        k_s[b * BLK : (b + 1) * BLK, :] = unit.astype(BF16)
        kt_s[:, b * BLK : (b + 1) * BLK] = unit.T.astype(BF16)

    def finish(p):
        slot = lax.rem(p, 2)
        for copy in cross_copies(p):
            copy.wait_recv()
        total = jnp.zeros((1, BLK), F32)
        for b in range(blocks):
            rows = slice(b * BLK, (b + 1) * BLK)
            hat, scale = normed(k_ref[rows, lanes_of(p)], ones)
            ext = slice(REACH + b * BLK, REACH + (b + 1) * BLK)
            dk, dv = dk_s[slot, ext, :], dv_s[slot, ext, :]
            back = b * BLK - (tokens - REACH)
            if back >= 0:
                dk = dk + bk_s[p, back : back + BLK, :].astype(F32)
                dv = dv + bv_s[p, back : back + BLK, :].astype(F32)
            total = total + jnp.sum(dk * hat, axis=0, keepdims=True)
            kg_ref[rows, lanes_of(p)] = norm_grad(dk, gain_k, hat, scale, ones).astype(BF16)
            vg_ref[rows, lanes_of(p)] = dv.astype(BF16)
        gk_s[...] += total

    def pair(p, _):
        slot = lax.rem(p, 2)
        for b in range(blocks):
            key_tile(k_ref[b * BLK : (b + 1) * BLK, lanes_of(p)], b + LEFT // 2)
        v_s[REACH:, :] = v_ref[:, lanes_of(p)]
        dk_s[slot] = jnp.zeros(dk_s.shape[1:], F32)
        dv_s[slot] = jnp.zeros(dv_s.shape[1:], F32)
        acc_s[...] = jnp.zeros_like(acc_s)
        clip_s[...] = jnp.zeros_like(clip_s)
        for head in range(2):
            build_bias(table_ref[pl.ds(p * 2 + head, 1), :], bias_s, head)

        def block(step, _):
            i = blocks - 1 - step

            @pl.when(step == blocks - LEFT // 2)
            def _():
                for copy in prior_copies(p):
                    copy.wait_recv()
                for b in range(LEFT // 2):
                    key_tile(pk_s[p, b * BLK : (b + 1) * BLK, :], b)
                v_s[:REACH, :] = pv_s[p]

            base = pl.multiple_of(i * BLK, BLK)
            rows = pl.ds(base, BLK)
            hat, scale = normed(q_ref[rows, lanes_of(p)], ones)
            qs = stack_halves((hat * gain_q).astype(BF16) * jnp.asarray(0.125, BF16))
            gs = stack_halves(g_ref[rows, lanes_of(p)])
            peaks, penalties = [], []
            for j in range(5):
                keys = pl.ds(base + j * BLK, BLK)
                own = slice(j * BLK, (j + 1) * BLK)
                s = dot(k_s[keys, :], qs, ((1,), (1,))) + bias_s[own, :]
                s_s[own, :] = s
                dw_s[own, :] = dot(v_s[keys, :], gs, ((1,), (1,)))
                penalty = jnp.where(first & (j < 4 - i), NEG, 0.0)
                penalties.append(penalty)
                peaks.append(jnp.max(s, axis=0, keepdims=True) + penalty)
            peak = functools.reduce(jnp.maximum, peaks)
            total = jnp.zeros((1, 2 * BLK), F32)
            delta = jnp.zeros((1, 2 * BLK), F32)
            for j in range(5):
                own = slice(j * BLK, (j + 1) * BLK)
                e = jnp.exp(s_s[own, :] - (peak - penalties[j]))
                s_s[own, :] = e
                total = total + jnp.sum(e, axis=0, keepdims=True)
                delta = delta + jnp.sum(e * dw_s[own, :], axis=0, keepdims=True)
            inverse = 1.0 / total
            delta = delta * inverse
            clipped = jnp.zeros((1, 2 * BLK), F32)
            for j in range(5):
                own = slice(j * BLK, (j + 1) * BLK)
                keys = pl.ds(base + j * BLK, BLK)
                w = s_s[own, :] * inverse
                ds = w * (dw_s[own, :] - delta)
                if j < 2:
                    clipped = clipped + jnp.sum(ds, axis=0, keepdims=True)
                else:
                    acc_s[(j - 2) * BLK : (j - 1) * BLK, :] += ds
                ds_low = ds.astype(BF16)
                ds_s[own, :] = ds_low
                dk_s[slot, keys, :] += dot(ds_low, qs, ((1,), (0,)))
                dv_s[slot, keys, :] += dot(w.astype(BF16), gs, ((1,), (0,)))
            clip_s[...] += clipped
            dqt = dot(kt_s[:, pl.ds(base, BAND)], ds_s[...], ((1,), (0,)))
            dqt = jnp.concatenate([dqt[:64, :BLK], dqt[64:, BLK:]], axis=0)
            dq = dqt.T * 0.125
            gq_s[...] += jnp.sum(dq * hat, axis=0, keepdims=True)
            qg_ref[rows, lanes_of(p)] = norm_grad(dq, gain_q, hat, scale, ones).astype(BF16)
            return 0

        lax.fori_loop(0, blocks, block, 0)
        ck_s[p] = dk_s[slot, :REACH, :].astype(BF16)
        cv_s[p] = dv_s[slot, :REACH, :].astype(BF16)
        lane = lax.broadcasted_iota(jnp.int32, (1, 512), 1)
        for head in range(2):
            far = jnp.sum(clip_s[:, head * BLK : (head + 1) * BLK], axis=1, keepdims=True)
            stat_s[0, pl.ds(p * 2 + head, 1), :] = fold_bias(acc_s, head) + jnp.where(lane == 0, far, 0.0)
        for copy in cross_copies(p):
            copy.start()

        @pl.when(p > 0)
        def _():
            finish(p - 1)

        return 0

    lax.fori_loop(0, pairs, pair, 0)
    finish(pairs - 1)
    rows = stat_s.shape[1]
    stat_s[0, rows - 8 : rows - 7, 0:BLK] = gq_s[...]
    stat_s[0, rows - 8 : rows - 7, BLK : 2 * BLK] = gk_s[...]
    for r, device in enumerate(partners):
        part = slice(0, rows) if r < len(doubling(sp)) else slice(rows - 8, rows)
        copy = remote(stat_s.at[r, part], got_s.at[r, part], stat_send.at[r], stat_recv.at[r], device)
        copy.start()
        copy.wait()
        stat_s[r + 1, part] = stat_s[r, part] + got_s[r, part]
    out_ref[: rows - 8, :] = stat_s[len(doubling(sp)), : rows - 8]
    out_ref[rows - 8 :, :] = stat_s[len(partners), rows - 8 :]
    for p in range(pairs):
        for copy in prior_copies(p) + cross_copies(p):
            copy.wait_send()


def body(query_rows, key_rows, value_rows, query_gain, key_gain, position_bias, output_grad):
    heads = position_bias.shape[0]
    pairs = heads // 2
    tokens = query_rows.shape[0]
    sp, tp = lax.axis_size("sp"), lax.axis_size("tp")
    rounds = len(doubling(sp)) + len(doubling(tp))
    table = position_bias.astype(F32)
    last = jnp.broadcast_to(table[:, -1:], (heads, 129))
    table = jnp.concatenate([last, jnp.full((heads, 64), NEG, F32), table[:, :-1]], axis=1)
    gains = jnp.stack([jnp.tile(query_gain.astype(F32), 2), jnp.tile(key_gain.astype(F32), 2)])
    ext = tokens + REACH
    rows = (heads + 7) // 8 * 8 + 8
    vmem = pl.BlockSpec(memory_space=pltpu.VMEM)
    grads = jax.ShapeDtypeStruct((tokens, heads * 64), BF16)
    sems = pltpu.SemaphoreType.DMA
    query_grad, key_grad, value_grad, stats = pl.pallas_call(
        functools.partial(kernel, sp, tp),
        in_specs=[vmem] * 6,
        out_specs=[vmem] * 4,
        out_shape=[grads, grads, grads, jax.ShapeDtypeStruct((rows, 512), F32)],
        scratch_shapes=[
            pltpu.VMEM((ext, BLK), BF16), pltpu.VMEM((BLK, ext), BF16), pltpu.VMEM((ext, BLK), BF16),
            pltpu.VMEM((BAND, 2 * BLK), F32), pltpu.VMEM((3 * BLK, 2 * BLK), F32),
            pltpu.VMEM((BAND, 2 * BLK), F32), pltpu.VMEM((BAND, 2 * BLK), F32),
            pltpu.VMEM((BAND, 2 * BLK), BF16),
            pltpu.VMEM((2, ext, BLK), F32), pltpu.VMEM((2, ext, BLK), F32),
            pltpu.VMEM((1, 2 * BLK), F32), pltpu.VMEM((1, BLK), F32), pltpu.VMEM((1, BLK), F32),
        ]
        + [pltpu.VMEM((pairs, REACH, BLK), BF16)] * 6
        + [
            pltpu.VMEM((rounds + 1, rows, 512), F32), pltpu.VMEM((rounds, rows, 512), F32),
            sems((2, pairs)), sems((2, pairs)), sems((2, pairs)), sems((2, pairs)),
            sems((rounds,)), sems((rounds,)),
        ],
        compiler_params=pltpu.CompilerParams(collective_id=0, has_side_effects=True, vmem_limit_bytes=48 << 20),
        name="attend",
    )(query_rows, key_rows, value_rows, output_grad, gains, table)
    fold = stats[:heads]
    bias_grad = jnp.concatenate([fold[:, 193:], jnp.sum(fold[:, :129], axis=1, keepdims=True)], axis=1)
    gain_row = stats[rows - 8]
    query_gain_grad = gain_row[:64] + gain_row[64:128]
    key_gain_grad = gain_row[128:192] + gain_row[192:256]
    return (query_grad, key_grad, value_grad, bias_grad, query_gain_grad, key_gain_grad)


def solution(mesh):
    placed = (P("sp", "tp"), P("sp", "tp"), P("sp", "tp"), P(), P(), P("tp", None), P("sp", "tp"))
    return jax.shard_map(
        body,
        mesh=mesh,
        in_specs=placed,
        out_specs=(P("sp", "tp"), P("sp", "tp"), P("sp", "tp"), P("tp", None), P(), P()),
        check_vma=False,
    )
```

```python
import functools

import jax
import jax.numpy as jnp
from jax import lax
from jax.experimental import pallas as pl
from jax.experimental.pallas import tpu as pltpu
from jax.sharding import PartitionSpec as P

SEG = 64
LEFT = 8
REACH = SEG * LEFT
RSPAN = 320
NORM_EPS = 1e-06
BLK = 2 * SEG
BAND = REACH + BLK
NEG = -1e30
F32 = jnp.float32
BF16 = jnp.bfloat16


def dot(a, b, dims):
    return lax.dot_general(a, b, (dims, ((), ())), preferred_element_type=F32)


def half_ones():
    row = lax.broadcasted_iota(jnp.int32, (BLK, BLK), 0) // 64
    col = lax.broadcasted_iota(jnp.int32, (BLK, BLK), 1) // 64
    return jnp.where(row == col, 1.0, 0.0).astype(BF16)


def head_mean(x, ones):
    high = x.astype(BF16)
    low = (x - high.astype(F32)).astype(BF16)
    return (dot(high, ones, ((1,), (0,))) + dot(low, ones, ((1,), (0,)))) * (1.0 / 64.0)


def normed(rows, ones):
    wide = rows.astype(F32)
    scale = lax.rsqrt(head_mean(wide * wide, ones) + NORM_EPS)
    return wide * scale, scale


def norm_grad(d_unit, gain, hat, scale, ones):
    scaled = d_unit * gain
    return scale * (scaled - hat * head_mean(scaled * hat, ones))


def stack_halves(x):
    lane = lax.broadcasted_iota(jnp.int32, x.shape, 1)
    zero = jnp.zeros_like(x)
    return jnp.concatenate([jnp.where(lane < 64, x, zero), jnp.where(lane < 64, zero, x)], axis=0)


def build_bias(table_row, bias_ref, head):
    wide = jnp.broadcast_to(table_row, (8, 512))
    sub = lax.broadcasted_iota(jnp.int32, (8, 512), 0)
    for bit in (1, 2, 4):
        wide = jnp.where((sub & bit) != 0, pltpu.roll(wide, bit, 1), wide)
    half = 8
    while half < BLK:
        wide = jnp.concatenate([wide, pltpu.roll(wide, half, 1)], axis=0)
        half *= 2
    lanes = slice(head * BLK, (head + 1) * BLK)
    row = lax.broadcasted_iota(jnp.int32, (BLK, BLK), 0)
    col = lax.broadcasted_iota(jnp.int32, (BLK, BLK), 1)
    far = jnp.broadcast_to(table_row[:, 0:1], (BLK, BLK))
    bias_ref[0:BLK, lanes] = jnp.where((row < SEG) & (col >= SEG), NEG, far)
    bias_ref[BLK : 2 * BLK, lanes] = far
    for j in range(3):
        tile = wide[:, ((4 - j) % 4) * BLK : ((4 - j) % 4) * BLK + BLK]
        if j == 2:
            tile = jnp.where((row >= SEG) & (col < SEG), NEG, tile)
        bias_ref[(2 + j) * BLK : (3 + j) * BLK, lanes] = tile


def fold_bias(acc_ref, head):
    lanes = slice(head * BLK, (head + 1) * BLK)
    tiles = [acc_ref[j * BLK : (j + 1) * BLK, lanes] for j in range(3)]
    wide = jnp.concatenate([tiles[0], jnp.zeros_like(tiles[0]), tiles[2], tiles[1]], axis=1)
    half = BLK // 2
    while half >= 8:
        wide = wide[:half] + pltpu.roll(wide[half:], 512 - half, 1)
        half //= 2
    for half in (4, 2, 1):
        wide = wide + pltpu.roll(pltpu.roll(wide, 512 - half, 1), 8 - half, 0)
    return wide[0:1]


def rounds_of(axis, size):
    rounds, stride = [], 1
    while stride < size:
        radix = 4 if size // stride % 4 == 0 else 2
        rounds.append((axis, stride, radix))
        stride *= radix
    return rounds


def peer(index, stride, radix, step):
    digit = (index // stride) % radix
    return index + stride * ((digit + step) % radix - digit)


def kernel(
    sp, tp, q_hbm, k_hbm, v_hbm, g_hbm, gains_ref, table_ref,
    qg_ref, kg_ref, vg_ref, out_ref,
    q_ref, k_ref, v_ref, g_ref,
    k_s, kt_s, v_s, bias_s, acc_s, s_s, dw_s, ds_s, w_s, qs_s, gs_s, hat_s, scale_s, dk_s, dv_s, clip_s, gq_s, gk_s,
    pk_s, pv_s, ck_s, cv_s, bk_s, bv_s, stat_s, got_s,
    prior_send, prior_recv, cross_send, cross_recv, stat_send, stat_recv, load_sem,
):
    tokens = q_ref.shape[0]
    blocks = tokens // BLK
    pairs = pk_s.shape[0]
    me = lax.axis_index("sp")
    me_tp = lax.axis_index("tp")
    right, left = lax.rem(me + 1, sp), lax.rem(me + sp - 1, sp)
    rounds = rounds_of("sp", sp) + rounds_of("tp", tp)
    peers = [
        [{axis: peer(me if axis == "sp" else me_tp, stride, radix, k)} for k in range(1, radix)]
        for axis, stride, radix in rounds
    ]
    first = me == 0

    def lanes_of(p):
        return pl.ds(pl.multiple_of(p * BLK, BLK), BLK)

    def loads(p):
        moves = ((k_hbm, k_ref), (q_hbm, q_ref), (v_hbm, v_ref), (g_hbm, g_ref))
        return [
            pltpu.make_async_copy(src.at[:, lanes_of(p)], dst.at[:, lanes_of(p)], load_sem.at[n, p])
            for n, (src, dst) in enumerate(moves)
        ]

    for p in range(pairs):
        for copy in loads(p):
            copy.start()

    barrier = pltpu.get_barrier_semaphore()
    greeted = [{"sp": right}, {"sp": left}] + [device for group in peers for device in group]
    for device in greeted:
        pl.semaphore_signal(barrier, inc=1, device_id=device, device_id_type=pl.DeviceIdType.MESH)
    pl.semaphore_wait(barrier, len(greeted))

    def remote(src, dst, send, recv, device):
        return pltpu.make_async_remote_copy(
            src_ref=src, dst_ref=dst, send_sem=send, recv_sem=recv,
            device_id=device, device_id_type=pl.DeviceIdType.MESH,
        )

    def prior_copies(p):
        rows = slice(tokens - REACH, tokens)
        return (
            remote(k_hbm.at[rows, lanes_of(p)], pk_s.at[p], prior_send.at[0, p], prior_recv.at[0, p], {"sp": right}),
            remote(v_hbm.at[rows, lanes_of(p)], pv_s.at[p], prior_send.at[1, p], prior_recv.at[1, p], {"sp": right}),
        )

    def cross_copies(p):
        return (
            remote(ck_s.at[p], bk_s.at[p], cross_send.at[0, p], cross_recv.at[0, p], {"sp": left}),
            remote(cv_s.at[p], bv_s.at[p], cross_send.at[1, p], cross_recv.at[1, p], {"sp": left}),
        )

    for p in range(pairs):
        for copy in prior_copies(p):
            copy.start()

    ones = half_ones()
    gain_q = gains_ref[0:1, :]
    gain_k = gains_ref[1:2, :]
    stat_s[0] = jnp.zeros(stat_s.shape[1:], F32)
    gq_s[...] = jnp.zeros_like(gq_s)
    gk_s[...] = jnp.zeros_like(gk_s)

    def key_tile(raw, b):
        unit = normed(raw, ones)[0] * gain_k
        k_s[b * BLK : (b + 1) * BLK, :] = unit.astype(BF16)
        kt_s[:, b * BLK : (b + 1) * BLK] = unit.T.astype(BF16)

    def finish(p):
        slot = lax.rem(p, 2)
        for copy in cross_copies(p):
            copy.wait_recv()
        total = jnp.zeros((1, BLK), F32)
        for b in range(blocks):
            rows = slice(b * BLK, (b + 1) * BLK)
            hat, scale = normed(k_ref[rows, lanes_of(p)], ones)
            ext = slice(REACH + b * BLK, REACH + (b + 1) * BLK)
            dk, dv = dk_s[slot, ext, :], dv_s[slot, ext, :]
            back = b * BLK - (tokens - REACH)
            if back >= 0:
                dk = dk + bk_s[p, back : back + BLK, :].astype(F32)
                dv = dv + bv_s[p, back : back + BLK, :].astype(F32)
            total = total + jnp.sum(dk * hat, axis=0, keepdims=True)
            kg_ref[rows, lanes_of(p)] = norm_grad(dk, gain_k, hat, scale, ones).astype(BF16)
            vg_ref[rows, lanes_of(p)] = dv.astype(BF16)
        gk_s[...] += total

    def pair(p, _):
        slot = lax.rem(p, 2)
        for head in range(2):
            build_bias(table_ref[pl.ds(p * 2 + head, 1), :], bias_s, head)
        dk_s[slot] = jnp.zeros(dk_s.shape[1:], F32)
        dv_s[slot] = jnp.zeros(dv_s.shape[1:], F32)
        acc_s[...] = jnp.zeros_like(acc_s)
        clip_s[...] = jnp.zeros_like(clip_s)
        for copy in loads(p):
            copy.wait()
        for b in range(blocks):
            rows = slice(b * BLK, (b + 1) * BLK)
            key_tile(k_ref[rows, lanes_of(p)], b + LEFT // 2)
            hat, scale = normed(q_ref[rows, lanes_of(p)], ones)
            hat_s[rows, :] = hat
            scale_s[rows, :] = scale
            qs_s[b] = stack_halves((hat * gain_q).astype(BF16) * jnp.asarray(0.125, BF16))
            gs_s[b] = stack_halves(g_ref[rows, lanes_of(p)])
        v_s[REACH:, :] = v_ref[:, lanes_of(p)]
        for copy in prior_copies(p):
            copy.wait_recv()
        for b in range(LEFT // 2):
            key_tile(pk_s[p, b * BLK : (b + 1) * BLK, :], b)
        v_s[:REACH, :] = pv_s[p]

        def tile(j):
            return slice(j * BLK, (j + 1) * BLK)

        def score(i, j, peaks):
            keys = tile(i + j)
            s = dot(k_s[keys, :], qs_s[i], ((1,), (1,))) + bias_s[tile(j), :]
            s_s[i % 2, tile(j), :] = s
            dw_s[i % 2, tile(j), :] = dot(v_s[keys, :], gs_s[i], ((1,), (1,)))
            top = jnp.max(s, axis=0, keepdims=True)
            peaks.append(top + penalty if j < LEFT // 2 - i else top)

        def product(i, j):
            keys = tile(i + j)
            dk_s[slot, keys, :] += dot(ds_s[i % 2, tile(j), :], qs_s[i], ((1,), (0,)))
            dv_s[slot, keys, :] += dot(w_s[i % 2, tile(j), :], gs_s[i], ((1,), (0,)))

        def query_side(i):
            rows = tile(i)
            dqt = dot(kt_s[:, i * BLK : i * BLK + BAND], ds_s[i % 2], ((1,), (0,)))
            dqt = jnp.concatenate([dqt[:64, :BLK], dqt[64:, BLK:]], axis=0)
            dq = dqt.T * 0.125
            hat = hat_s[rows, :]
            gq_s[...] += jnp.sum(dq * hat, axis=0, keepdims=True)
            qg_ref[rows, lanes_of(p)] = norm_grad(dq, gain_q, hat, scale_s[rows, :], ones).astype(BF16)

        penalty = jnp.where(first, NEG, 0.0)
        peaks = {}
        for step in range(blocks + 2):
            ahead, here, behind = step, step - 1, step - 2
            peaks[ahead] = []
            if 0 <= here < blocks:
                peak = functools.reduce(jnp.maximum, peaks[here])
                total = jnp.zeros((1, 2 * BLK), F32)
                delta = jnp.zeros((1, 2 * BLK), F32)
                clipped = jnp.zeros((1, 2 * BLK), F32)
            for j in range(5):
                if ahead < blocks:
                    score(ahead, j, peaks[ahead])
                if 0 <= here < blocks:
                    e = jnp.exp(s_s[here % 2, tile(j), :] - (peak - penalty if j < LEFT // 2 - here else peak))
                    s_s[here % 2, tile(j), :] = e
                    total = total + jnp.sum(e, axis=0, keepdims=True)
                    delta = delta + jnp.sum(e * dw_s[here % 2, tile(j), :], axis=0, keepdims=True)
            if 0 <= here < blocks:
                inverse = 1.0 / total
                delta = delta * inverse
            if behind >= 0:
                query_side(behind)
            for j in range(5):
                if behind >= 0:
                    product(behind, j)
                if 0 <= here < blocks:
                    w = s_s[here % 2, tile(j), :] * inverse
                    ds = w * (dw_s[here % 2, tile(j), :] - delta)
                    if j < 2:
                        clipped = clipped + jnp.sum(ds, axis=0, keepdims=True)
                    else:
                        acc_s[tile(j - 2), :] += ds
                    ds_s[here % 2, tile(j), :] = ds.astype(BF16)
                    w_s[here % 2, tile(j), :] = w.astype(BF16)
            if 0 <= here < blocks:
                clip_s[...] += clipped
        ck_s[p] = dk_s[slot, :REACH, :].astype(BF16)
        cv_s[p] = dv_s[slot, :REACH, :].astype(BF16)
        lane = lax.broadcasted_iota(jnp.int32, (1, 512), 1)
        for head in range(2):
            far = jnp.sum(clip_s[:, head * BLK : (head + 1) * BLK], axis=1, keepdims=True)
            stat_s[0, pl.ds(p * 2 + head, 1), :] = fold_bias(acc_s, head) + jnp.where(lane == 0, far, 0.0)
        for copy in cross_copies(p):
            copy.start()

        @pl.when(p > 0)
        def _():
            finish(p - 1)

        return 0

    lax.fori_loop(0, pairs, pair, 0)
    finish(pairs - 1)
    rows = stat_s.shape[1]
    stat_s[0, rows - 8 : rows - 7, 0:BLK] = gq_s[...]
    stat_s[0, rows - 8 : rows - 7, BLK : 2 * BLK] = gk_s[...]
    summed = len(rounds_of("sp", sp))
    for r, group in enumerate(peers):
        part = slice(0, rows) if r < summed else slice(rows - 8, rows)
        copies = [
            remote(stat_s.at[r, part], got_s.at[r, k, part], stat_send.at[r, k], stat_recv.at[r, k], device)
            for k, device in enumerate(group)
        ]
        for copy in copies:
            copy.start()
        for copy in copies:
            copy.wait()
        if len(group) == 3:
            stat_s[r + 1, part] = (stat_s[r, part] + got_s[r, 1, part]) + (got_s[r, 0, part] + got_s[r, 2, part])
        else:
            stat_s[r + 1, part] = stat_s[r, part] + got_s[r, 0, part]
    out_ref[: rows - 8, :] = stat_s[summed, : rows - 8]
    out_ref[rows - 8 :, :] = stat_s[len(peers), rows - 8 :]
    for p in range(pairs):
        for copy in prior_copies(p) + cross_copies(p):
            copy.wait_send()


def body(query_rows, key_rows, value_rows, query_gain, key_gain, position_bias, output_grad):
    heads = position_bias.shape[0]
    pairs = heads // 2
    tokens = query_rows.shape[0]
    sp, tp = lax.axis_size("sp"), lax.axis_size("tp")
    rounds = len(rounds_of("sp", sp) + rounds_of("tp", tp))
    table = position_bias.astype(F32)
    last = jnp.broadcast_to(table[:, -1:], (heads, 129))
    table = jnp.concatenate([last, jnp.full((heads, 64), NEG, F32), table[:, :-1]], axis=1)
    gains = jnp.stack([jnp.tile(query_gain.astype(F32), 2), jnp.tile(key_gain.astype(F32), 2)])
    ext = tokens + REACH
    rows = (heads + 7) // 8 * 8 + 8
    vmem = pl.BlockSpec(memory_space=pltpu.VMEM)
    grads = jax.ShapeDtypeStruct((tokens, heads * 64), BF16)
    sems = pltpu.SemaphoreType.DMA
    query_grad, key_grad, value_grad, stats = pl.pallas_call(
        functools.partial(kernel, sp, tp),
        in_specs=[pl.BlockSpec(memory_space=pltpu.HBM)] * 4 + [vmem] * 2,
        out_specs=[vmem] * 4,
        out_shape=[grads, grads, grads, jax.ShapeDtypeStruct((rows, 512), F32)],
        scratch_shapes=[pltpu.VMEM((tokens, heads * 64), BF16)] * 4
        + [
            pltpu.VMEM((ext, BLK), BF16), pltpu.VMEM((BLK, ext), BF16), pltpu.VMEM((ext, BLK), BF16),
            pltpu.VMEM((BAND, 2 * BLK), F32), pltpu.VMEM((3 * BLK, 2 * BLK), F32),
            pltpu.VMEM((2, BAND, 2 * BLK), F32), pltpu.VMEM((2, BAND, 2 * BLK), F32),
            pltpu.VMEM((2, BAND, 2 * BLK), BF16), pltpu.VMEM((2, BAND, 2 * BLK), BF16),
            pltpu.VMEM((tokens // BLK, 2 * BLK, BLK), BF16), pltpu.VMEM((tokens // BLK, 2 * BLK, BLK), BF16),
            pltpu.VMEM((tokens, BLK), F32), pltpu.VMEM((tokens, BLK), F32),
            pltpu.VMEM((2, ext, BLK), F32), pltpu.VMEM((2, ext, BLK), F32),
            pltpu.VMEM((1, 2 * BLK), F32), pltpu.VMEM((1, BLK), F32), pltpu.VMEM((1, BLK), F32),
        ]
        + [pltpu.VMEM((pairs, REACH, BLK), BF16)] * 6
        + [
            pltpu.VMEM((rounds + 1, rows, 512), F32), pltpu.VMEM((rounds, 3, rows, 512), F32),
            sems((2, pairs)), sems((2, pairs)), sems((2, pairs)), sems((2, pairs)),
            sems((rounds, 3)), sems((rounds, 3)), sems((4, pairs)),
        ],
        compiler_params=pltpu.CompilerParams(collective_id=0, has_side_effects=True, vmem_limit_bytes=48 << 20),
        name="attend",
    )(query_rows, key_rows, value_rows, output_grad, gains, table)
    fold = stats[:heads]
    bias_grad = jnp.concatenate([fold[:, 193:], jnp.sum(fold[:, :129], axis=1, keepdims=True)], axis=1)
    gain_row = stats[rows - 8]
    query_gain_grad = gain_row[:64] + gain_row[64:128]
    key_gain_grad = gain_row[128:192] + gain_row[192:256]
    return (query_grad, key_grad, value_grad, bias_grad, query_gain_grad, key_gain_grad)


def solution(mesh):
    placed = (P("sp", "tp"), P("sp", "tp"), P("sp", "tp"), P(), P(), P("tp", None), P("sp", "tp"))
    return jax.shard_map(
        body,
        mesh=mesh,
        in_specs=placed,
        out_specs=(P("sp", "tp"), P("sp", "tp"), P("sp", "tp"), P("tp", None), P(), P()),
        check_vma=False,
    )
```

```python
import functools

import jax
import jax.numpy as jnp
from jax import lax
from jax.experimental import pallas as pl
from jax.experimental.pallas import tpu as pltpu
from jax.sharding import PartitionSpec as P

SEG = 64
LEFT = 8
REACH = SEG * LEFT
RSPAN = 320
NORM_EPS = 1e-06
BLK = 2 * SEG
BAND = REACH + BLK
NEG = -1e30
F32 = jnp.float32
BF16 = jnp.bfloat16


def dot(a, b, dims):
    return lax.dot_general(a, b, (dims, ((), ())), preferred_element_type=F32)


def half_ones():
    row = lax.broadcasted_iota(jnp.int32, (BLK, BLK), 0) // 64
    col = lax.broadcasted_iota(jnp.int32, (BLK, BLK), 1) // 64
    return jnp.where(row == col, 1.0, 0.0).astype(BF16)


def head_mean(x, ones):
    high = x.astype(BF16)
    low = (x - high.astype(F32)).astype(BF16)
    return (dot(high, ones, ((1,), (0,))) + dot(low, ones, ((1,), (0,)))) * (1.0 / 64.0)


def normed(rows, ones):
    wide = rows.astype(F32)
    scale = lax.rsqrt(head_mean(wide * wide, ones) + NORM_EPS)
    return wide * scale, scale


def norm_grad(d_unit, gain, hat, scale, ones):
    scaled = d_unit * gain
    return scale * (scaled - hat * head_mean(scaled * hat, ones))


def stack_halves(x):
    lane = lax.broadcasted_iota(jnp.int32, x.shape, 1)
    zero = jnp.zeros_like(x)
    return jnp.concatenate([jnp.where(lane < 64, x, zero), jnp.where(lane < 64, zero, x)], axis=0)


def build_bias(table_row, bias_ref, head):
    wide = jnp.broadcast_to(table_row, (8, 512))
    sub = lax.broadcasted_iota(jnp.int32, (8, 512), 0)
    for bit in (1, 2, 4):
        wide = jnp.where((sub & bit) != 0, pltpu.roll(wide, bit, 1), wide)
    half = 8
    while half < BLK:
        wide = jnp.concatenate([wide, pltpu.roll(wide, half, 1)], axis=0)
        half *= 2
    lanes = slice(head * BLK, (head + 1) * BLK)
    row = lax.broadcasted_iota(jnp.int32, (BLK, BLK), 0)
    col = lax.broadcasted_iota(jnp.int32, (BLK, BLK), 1)
    far = jnp.broadcast_to(table_row[:, 0:1], (BLK, BLK))
    bias_ref[0:BLK, lanes] = jnp.where((row < SEG) & (col >= SEG), NEG, far)
    bias_ref[BLK : 2 * BLK, lanes] = far
    for j in range(3):
        tile = wide[:, ((4 - j) % 4) * BLK : ((4 - j) % 4) * BLK + BLK]
        if j == 2:
            tile = jnp.where((row >= SEG) & (col < SEG), NEG, tile)
        bias_ref[(2 + j) * BLK : (3 + j) * BLK, lanes] = tile


def fold_bias(acc_ref, head):
    lanes = slice(head * BLK, (head + 1) * BLK)
    tiles = [acc_ref[j * BLK : (j + 1) * BLK, lanes] for j in range(3)]
    wide = jnp.concatenate([tiles[0], jnp.zeros_like(tiles[0]), tiles[2], tiles[1]], axis=1)
    half = BLK // 2
    while half >= 8:
        wide = wide[:half] + pltpu.roll(wide[half:], 512 - half, 1)
        half //= 2
    for half in (4, 2, 1):
        wide = wide + pltpu.roll(pltpu.roll(wide, 512 - half, 1), 8 - half, 0)
    return wide[0:1]


def rounds_of(axis, size):
    rounds, stride = [], 1
    while stride < size:
        radix = 4 if size // stride % 4 == 0 else 2
        rounds.append((axis, stride, radix))
        stride *= radix
    return rounds


def peer(index, stride, radix, step):
    digit = (index // stride) % radix
    return index + stride * ((digit + step) % radix - digit)


def kernel(
    sp, tp, q_hbm, k_hbm, v_hbm, g_hbm, gains_ref, table_ref,
    qg_ref, kg_ref, vg_ref, out_ref,
    q_ref, k_ref, v_ref, g_ref,
    k_s, kt_s, v_s, bias_s, acc_s, s_s, dw_s, ds_s, w_s, qs_s, gs_s, hat_s, scale_s, dk_s, dv_s, clip_s, gq_s, gk_s,
    pk_s, pv_s, ck_s, cv_s, bk_s, bv_s, stat_s, got_s,
    prior_send, prior_recv, cross_send, cross_recv, stat_send, stat_recv, load_sem,
):
    tokens = q_ref.shape[0]
    blocks = tokens // BLK
    pairs = pk_s.shape[0]
    me = lax.axis_index("sp")
    me_tp = lax.axis_index("tp")
    right, left = lax.rem(me + 1, sp), lax.rem(me + sp - 1, sp)
    rounds = rounds_of("sp", sp) + rounds_of("tp", tp)
    peers = [
        [{axis: peer(me if axis == "sp" else me_tp, stride, radix, k)} for k in range(1, radix)]
        for axis, stride, radix in rounds
    ]
    first = me == 0

    def lanes_of(p):
        return pl.ds(pl.multiple_of(p * BLK, BLK), BLK)

    def loads(p):
        moves = ((k_hbm, k_ref), (q_hbm, q_ref), (v_hbm, v_ref), (g_hbm, g_ref))
        return [
            pltpu.make_async_copy(src.at[:, lanes_of(p)], dst.at[:, lanes_of(p)], load_sem.at[n, p])
            for n, (src, dst) in enumerate(moves)
        ]

    for p in range(pairs):
        for copy in loads(p):
            copy.start()

    barrier = pltpu.get_barrier_semaphore()
    greeted = [{"sp": right}, {"sp": left}] + [device for group in peers for device in group]
    for device in greeted:
        pl.semaphore_signal(barrier, inc=1, device_id=device, device_id_type=pl.DeviceIdType.MESH)
    pl.semaphore_wait(barrier, len(greeted))

    def remote(src, dst, send, recv, device):
        return pltpu.make_async_remote_copy(
            src_ref=src, dst_ref=dst, send_sem=send, recv_sem=recv,
            device_id=device, device_id_type=pl.DeviceIdType.MESH,
        )

    def prior_copies(p):
        rows = slice(tokens - REACH, tokens)
        return (
            remote(k_hbm.at[rows, lanes_of(p)], pk_s.at[p], prior_send.at[0, p], prior_recv.at[0, p], {"sp": right}),
            remote(v_hbm.at[rows, lanes_of(p)], pv_s.at[p], prior_send.at[1, p], prior_recv.at[1, p], {"sp": right}),
        )

    def cross_copies(p):
        return (
            remote(ck_s.at[p], bk_s.at[p], cross_send.at[0, p], cross_recv.at[0, p], {"sp": left}),
            remote(cv_s.at[p], bv_s.at[p], cross_send.at[1, p], cross_recv.at[1, p], {"sp": left}),
        )

    for p in range(pairs):
        for copy in prior_copies(p):
            copy.start()

    ones = half_ones()
    gain_q = gains_ref[0:1, :]
    gain_k = gains_ref[1:2, :]
    stat_s[0] = jnp.zeros(stat_s.shape[1:], F32)
    gq_s[...] = jnp.zeros_like(gq_s)
    gk_s[...] = jnp.zeros_like(gk_s)

    def key_tile(raw, b):
        unit = normed(raw, ones)[0] * gain_k
        k_s[b * BLK : (b + 1) * BLK, :] = unit.astype(BF16)
        kt_s[:, b * BLK : (b + 1) * BLK] = unit.T.astype(BF16)

    def finish(p):
        slot = lax.rem(p, 2)
        for copy in cross_copies(p):
            copy.wait_recv()
        total = jnp.zeros((1, BLK), F32)
        for b in range(blocks):
            rows = slice(b * BLK, (b + 1) * BLK)
            hat, scale = normed(k_ref[rows, lanes_of(p)], ones)
            ext = slice(REACH + b * BLK, REACH + (b + 1) * BLK)
            dk, dv = dk_s[slot, ext, :], dv_s[slot, ext, :]
            back = b * BLK - (tokens - REACH)
            if back >= 0:
                dk = dk + bk_s[p, back : back + BLK, :].astype(F32)
                dv = dv + bv_s[p, back : back + BLK, :].astype(F32)
            total = total + jnp.sum(dk * hat, axis=0, keepdims=True)
            kg_ref[rows, lanes_of(p)] = norm_grad(dk, gain_k, hat, scale, ones).astype(BF16)
            vg_ref[rows, lanes_of(p)] = dv.astype(BF16)
        gk_s[...] += total

    def pair(p, _):
        slot = lax.rem(p, 2)
        for head in range(2):
            build_bias(table_ref[pl.ds(p * 2 + head, 1), :], bias_s, head)
        dk_s[slot] = jnp.zeros(dk_s.shape[1:], F32)
        dv_s[slot] = jnp.zeros(dv_s.shape[1:], F32)
        acc_s[...] = jnp.zeros_like(acc_s)
        clip_s[...] = jnp.zeros_like(clip_s)
        for copy in loads(p):
            copy.wait()
        for b in range(blocks):
            rows = slice(b * BLK, (b + 1) * BLK)
            key_tile(k_ref[rows, lanes_of(p)], b + LEFT // 2)
            hat, scale = normed(q_ref[rows, lanes_of(p)], ones)
            hat_s[rows, :] = hat
            scale_s[rows, :] = scale
            qs_s[b] = stack_halves((hat * gain_q).astype(BF16) * jnp.asarray(0.125, BF16))
            gs_s[b] = stack_halves(g_ref[rows, lanes_of(p)])
        v_s[REACH:, :] = v_ref[:, lanes_of(p)]
        for copy in prior_copies(p):
            copy.wait_recv()
        for b in range(LEFT // 2):
            key_tile(pk_s[p, b * BLK : (b + 1) * BLK, :], b)
        v_s[:REACH, :] = pv_s[p]

        def tile(j):
            return slice(j * BLK, (j + 1) * BLK)

        def score(i, j, peaks):
            keys = tile(i + j)
            s = dot(k_s[keys, :], qs_s[i], ((1,), (1,))) + bias_s[tile(j), :]
            s_s[i % 2, tile(j), :] = s
            dw_s[i % 2, tile(j), :] = dot(v_s[keys, :], gs_s[i], ((1,), (1,)))
            top = jnp.max(s, axis=0, keepdims=True)
            peaks.append(top + penalty if j < LEFT // 2 - i else top)

        def product(i, j):
            keys = tile(i + j)
            dk_s[slot, keys, :] += dot(ds_s[i % 2, tile(j), :], qs_s[i], ((1,), (0,)))
            dv_s[slot, keys, :] += dot(w_s[i % 2, tile(j), :], gs_s[i], ((1,), (0,)))

        def query_side(i):
            rows = tile(i)
            dqt = dot(kt_s[:, i * BLK : i * BLK + BAND], ds_s[i % 2], ((1,), (0,)))
            dqt = jnp.concatenate([dqt[:64, :BLK], dqt[64:, BLK:]], axis=0)
            dq = dqt.T * 0.125
            hat = hat_s[rows, :]
            gq_s[...] += jnp.sum(dq * hat, axis=0, keepdims=True)
            qg_ref[rows, lanes_of(p)] = norm_grad(dq, gain_q, hat, scale_s[rows, :], ones).astype(BF16)

        penalty = jnp.where(first, NEG, 0.0)
        peaks = {}
        for step in range(blocks + 2):
            ahead, here, behind = step, step - 1, step - 2
            peaks[ahead] = []
            if 0 <= here < blocks:
                peak = functools.reduce(jnp.maximum, peaks[here])
                total = jnp.zeros((1, 2 * BLK), F32)
                delta = jnp.zeros((1, 2 * BLK), F32)
                clipped = jnp.zeros((1, 2 * BLK), F32)
            for j in range(5):
                if ahead < blocks:
                    score(ahead, j, peaks[ahead])
                if 0 <= here < blocks:
                    e = jnp.exp(s_s[here % 2, tile(j), :] - (peak - penalty if j < LEFT // 2 - here else peak))
                    s_s[here % 2, tile(j), :] = e
                    total = total + jnp.sum(e, axis=0, keepdims=True)
                    delta = delta + jnp.sum(e * dw_s[here % 2, tile(j), :], axis=0, keepdims=True)
            if 0 <= here < blocks:
                inverse = 1.0 / total
                delta = delta * inverse
            if behind >= 0:
                query_side(behind)
            for j in range(5):
                if behind >= 0:
                    product(behind, j)
                if 0 <= here < blocks:
                    w = s_s[here % 2, tile(j), :] * inverse
                    ds = w * (dw_s[here % 2, tile(j), :] - delta)
                    if j < 2:
                        clipped = clipped + jnp.sum(ds, axis=0, keepdims=True)
                    else:
                        acc_s[tile(j - 2), :] += ds
                    ds_s[here % 2, tile(j), :] = ds.astype(BF16)
                    w_s[here % 2, tile(j), :] = w.astype(BF16)
            if 0 <= here < blocks:
                clip_s[...] += clipped
        ck_s[p] = dk_s[slot, :REACH, :].astype(BF16)
        cv_s[p] = dv_s[slot, :REACH, :].astype(BF16)
        lane = lax.broadcasted_iota(jnp.int32, (1, 512), 1)
        for head in range(2):
            far = jnp.sum(clip_s[:, head * BLK : (head + 1) * BLK], axis=1, keepdims=True)
            stat_s[0, pl.ds(p * 2 + head, 1), :] = fold_bias(acc_s, head) + jnp.where(lane == 0, far, 0.0)
        for copy in cross_copies(p):
            copy.start()

        @pl.when(p > 0)
        def _():
            finish(p - 1)

        return 0

    lax.fori_loop(0, pairs, pair, 0)
    finish(pairs - 1)
    rows = stat_s.shape[1]
    stat_s[0, rows - 8 : rows - 7, 0:BLK] = gq_s[...]
    stat_s[0, rows - 8 : rows - 7, BLK : 2 * BLK] = gk_s[...]
    summed = len(rounds_of("sp", sp))
    for r, group in enumerate(peers):
        part = slice(0, rows) if r < summed else slice(rows - 8, rows)
        copies = [
            remote(stat_s.at[r, part], got_s.at[r, k, part], stat_send.at[r, k], stat_recv.at[r, k], device)
            for k, device in enumerate(group)
        ]
        for copy in copies:
            copy.start()
        for copy in copies:
            copy.wait()
        if len(group) == 3:
            stat_s[r + 1, part] = (stat_s[r, part] + got_s[r, 1, part]) + (got_s[r, 0, part] + got_s[r, 2, part])
        else:
            stat_s[r + 1, part] = stat_s[r, part] + got_s[r, 0, part]
    out_ref[: rows - 8, :] = stat_s[summed, : rows - 8]
    out_ref[rows - 8 :, :] = stat_s[len(peers), rows - 8 :]
    for p in range(pairs):
        for copy in prior_copies(p) + cross_copies(p):
            copy.wait_send()


def body(query_rows, key_rows, value_rows, query_gain, key_gain, position_bias, output_grad):
    heads = position_bias.shape[0]
    pairs = heads // 2
    tokens = query_rows.shape[0]
    sp, tp = lax.axis_size("sp"), lax.axis_size("tp")
    rounds = len(rounds_of("sp", sp) + rounds_of("tp", tp))
    table = position_bias.astype(F32)
    last = jnp.broadcast_to(table[:, -1:], (heads, 129))
    table = jnp.concatenate([last, jnp.full((heads, 64), NEG, F32), table[:, :-1]], axis=1)
    gains = jnp.stack([jnp.tile(query_gain.astype(F32), 2), jnp.tile(key_gain.astype(F32), 2)])
    ext = tokens + REACH
    rows = (heads + 7) // 8 * 8 + 8
    vmem = pl.BlockSpec(memory_space=pltpu.VMEM)
    grads = jax.ShapeDtypeStruct((tokens, heads * 64), BF16)
    sems = pltpu.SemaphoreType.DMA
    query_grad, key_grad, value_grad, stats = pl.pallas_call(
        functools.partial(kernel, sp, tp),
        in_specs=[pl.BlockSpec(memory_space=pltpu.HBM)] * 4 + [vmem] * 2,
        out_specs=[vmem] * 4,
        out_shape=[grads, grads, grads, jax.ShapeDtypeStruct((rows, 512), F32)],
        scratch_shapes=[pltpu.VMEM((tokens, heads * 64), BF16)] * 4
        + [
            pltpu.VMEM((ext, BLK), BF16), pltpu.VMEM((BLK, ext), BF16), pltpu.VMEM((ext, BLK), BF16),
            pltpu.VMEM((BAND, 2 * BLK), F32), pltpu.VMEM((3 * BLK, 2 * BLK), F32),
            pltpu.VMEM((2, BAND, 2 * BLK), F32), pltpu.VMEM((2, BAND, 2 * BLK), F32),
            pltpu.VMEM((2, BAND, 2 * BLK), BF16), pltpu.VMEM((2, BAND, 2 * BLK), BF16),
            pltpu.VMEM((tokens // BLK, 2 * BLK, BLK), BF16), pltpu.VMEM((tokens // BLK, 2 * BLK, BLK), BF16),
            pltpu.VMEM((tokens, BLK), F32), pltpu.VMEM((tokens, BLK), F32),
            pltpu.VMEM((2, ext, BLK), F32), pltpu.VMEM((2, ext, BLK), F32),
            pltpu.VMEM((1, 2 * BLK), F32), pltpu.VMEM((1, BLK), F32), pltpu.VMEM((1, BLK), F32),
        ]
        + [pltpu.VMEM((pairs, REACH, BLK), BF16)] * 6
        + [
            pltpu.VMEM((rounds + 1, rows, 512), F32), pltpu.VMEM((rounds, 3, rows, 512), F32),
            sems((2, pairs)), sems((2, pairs)), sems((2, pairs)), sems((2, pairs)),
            sems((rounds, 3)), sems((rounds, 3)), sems((4, pairs)),
        ],
        compiler_params=pltpu.CompilerParams(collective_id=0, has_side_effects=True, vmem_limit_bytes=67_043_328),
        name="attend",
    )(query_rows, key_rows, value_rows, output_grad, gains, table)
    fold = stats[:heads]
    bias_grad = jnp.concatenate([fold[:, 193:], jnp.sum(fold[:, :129], axis=1, keepdims=True)], axis=1)
    gain_row = stats[rows - 8]
    query_gain_grad = gain_row[:64] + gain_row[64:128]
    key_gain_grad = gain_row[128:192] + gain_row[192:256]
    return (query_grad, key_grad, value_grad, bias_grad, query_gain_grad, key_gain_grad)


def solution(mesh):
    placed = (P("sp", "tp"), P("sp", "tp"), P("sp", "tp"), P(), P(), P("tp", None), P("sp", "tp"))
    return jax.shard_map(
        body,
        mesh=mesh,
        in_specs=placed,
        out_specs=(P("sp", "tp"), P("sp", "tp"), P("sp", "tp"), P("tp", None), P(), P()),
        check_vma=False,
    )
```
